32 devices in a mesh: kv: 8 (over z, y), tp: 4 (over x, core).
Axes of the slice: x: 2, y: 2, z: 4, core: 2. Of those that a mesh axis runs over, the one named last changes fastest.
Arguments:
- query_rows: bfloat16 [16384, 1536], P('kv', 'tp'), may hold values from -6 to 6
- key_rows: bfloat16 [16384, 1536], P('kv', 'tp'), may hold values from -6 to 6
- value_rows: bfloat16 [16384, 1536], P('kv', 'tp'), may hold values from -6 to 6
- log_sums: float32 [12, 16384], P('tp', 'kv'), may hold values from 5.5 to 7.5
- cotangent: bfloat16 [16384, 1536], P('kv', 'tp'), may hold values from -24 to 24
- layer_input: bfloat16 [16384, 4096], P('kv', 'tp'), may hold values from -0.29882812 to 0.29882812
- chosen: int32 [12, 512, 12], P('tp'), may hold values from -1 to 447, as said below
Outputs:
- grad_queries: bfloat16 [16384, 1536], P('kv', 'tp')
- grad_keys: float32 [16384, 1536], P('kv', 'tp')
- grad_values: float32 [16384, 1536], P('kv', 'tp')
- grad_weight: float32 [4096, 1536], P(('tp', 'kv'))
The draws below stay inside these ranges and needn't reach their ends.
Inputs may be any that keep to these rules, and one draw needn't show every extreme that they name: `chosen`: for query block i, write j = i // 64. Every entry other than -1 names a block below j * 64; the entries of a row are distinct, the -1 entries stand last, and a row has exactly min(12, 2 * min(j, 7)) entries other than -1. For one head, the rows with the same j name at most 2 distinct blocks of any one span; for j >= 1 the span j - 1 gives exactly 2 blocks, named by every such row.
All inputs are finite; a program needn't handle non-finite values.
Results may differ from the reference program's by a relative error of at most 0.007.
Values may be sent and summed in bfloat16 or wider, within the bound.
A program may use at most 192 MiB of HBM per device.

```python
import jax
import jax.numpy as jnp
from jax import lax

D = 4096
HEADS = 12
HEAD_DIM = 128
KEY_BLOCK = 32
SEL = 12
CAP = 2
OWNERS = 7
TOKENS = 16384
BPD = 64
N_KV = 8


def draw_chosen(key, part):
    base_key = jax.random.fold_in(key, 17)
    owner_key, block_key, row_key = jax.random.split(base_key, 3)
    asking_accelerator = jnp.arange(N_KV, dtype=jnp.int32)[:, None]
    proposed_segment = jnp.arange(N_KV, dtype=jnp.int32)[None, :]
    noise_perturbation = jax.random.randint(owner_key, (HEADS, N_KV, N_KV), 0, 1 << 20, dtype=jnp.int32) * 64 + proposed_segment
    merit_increment = jnp.where(proposed_segment == asking_accelerator - 1, 3 << 27, jnp.where(proposed_segment == asking_accelerator - N_KV // 2, 2 << 27, jnp.where(proposed_segment == 0, 1 << 27, 0)))
    possessor_merit = jnp.where(proposed_segment < asking_accelerator, noise_perturbation + merit_increment, -1 - proposed_segment)
    owner_top, owner_pick = lax.top_k(possessor_merit, OWNERS)
    owner_valid = owner_top >= 0
    block_noise = jax.random.randint(block_key, (HEADS, N_KV, OWNERS, BPD), 0, 1 << 20, dtype=jnp.int32) * BPD + jnp.arange(BPD, dtype=jnp.int32)
    block_top, block_pick = lax.top_k(block_noise, CAP)
    pool_ids = (owner_pick[:, :, :, None] * BPD + block_pick).reshape(HEADS, N_KV, OWNERS * CAP)
    pool_valid = jnp.repeat(owner_valid, CAP, axis=2)
    pool_size = OWNERS * CAP
    slot_ids = jnp.arange(pool_size, dtype=jnp.int32)
    row_noise = jax.random.randint(row_key, (HEADS, N_KV, BPD, pool_size), 0, 1 << 20, dtype=jnp.int32) * pool_size + slot_ids
    row_noise = row_noise + jnp.where(slot_ids < 2 * CAP, 1 << 27, 0)
    row_score = jnp.where(pool_valid[:, :, None, :], row_noise, -1 - slot_ids)
    row_top, row_pick = lax.top_k(row_score, SEL)
    picked = jnp.take_along_axis(jnp.broadcast_to(pool_ids[:, :, None, :], row_score.shape), row_pick, axis=3)
    result = jnp.where(row_top >= 0, picked, -1)
    return result.reshape(HEADS, N_KV * BPD, SEL).astype(jnp.int32)


def block_levels(stream_key, shape, shards, smallest, high):
    level, own = 1.0, jax.random.fold_in(stream_key, 6)
    for dim, blocks in shards:
        heights = jnp.exp(jax.random.uniform(jax.random.fold_in(own, dim), (blocks,), jnp.float32, smallest / len(shards), high / len(shards)))
        level = level * jnp.repeat(heights, shape[dim] // blocks).reshape([-1 if axis == dim else 1 for axis in range(len(shape))])
    return level


def gaussian(own_key, shape, deviation, most, cuts=(), kind=jnp.bfloat16):
    entries = deviation * jax.random.normal(own_key, shape, jnp.float32)
    if cuts:
        entries = entries * block_levels(own_key, shape, cuts, -0.22, 0.18)
    return jnp.clip(entries, -most, most).astype(kind)


def setup_inputs(seed: int = 0) -> dict:
    seeds = jax.random.split(jax.random.key(seed), 8)
    return {
        "query_rows": gaussian(seeds[0], (TOKENS, HEADS * HEAD_DIM), 1.0, 6.0, ((0, 8), (1, 4))),
        "key_rows": gaussian(seeds[1], (TOKENS, HEADS * HEAD_DIM), 1.0, 6.0, ((0, 8), (1, 4))),
        "value_rows": gaussian(seeds[2], (TOKENS, HEADS * HEAD_DIM), 1.0, 6.0, ((0, 8), (1, 4))),
        "log_sums": jnp.clip(5.5 + 2.0 * jax.random.uniform(seeds[3], (HEADS, TOKENS), jnp.float32) ** block_levels(seeds[3], (HEADS, TOKENS), ((0, 4), (1, 8)), -0.2, 0.2), 5.5, 7.5),
        "cotangent": gaussian(seeds[4], (TOKENS, HEADS * HEAD_DIM), 4.0, 24.0, ((0, 8), (1, 4))),
        "layer_input": gaussian(seeds[5], (TOKENS, D), 0.05, 0.29882812, ((0, 8), (1, 4))),
        "chosen": draw_chosen(jax.random.fold_in(seeds[7], 71), 0),
    }


def head_grads(inputs):
    query_portion, key_part, value_part, output_gradient, log_sum, picked = inputs
    blocks = query_portion.shape[0] // KEY_BLOCK
    scale_factor = HEAD_DIM ** -0.5
    batch_query = query_portion.reshape(blocks, KEY_BLOCK, HEAD_DIM).astype(jnp.float32)
    key_b = key_part.reshape(blocks, KEY_BLOCK, HEAD_DIM).astype(jnp.float32)
    value_b = value_part.reshape(blocks, KEY_BLOCK, HEAD_DIM).astype(jnp.float32)
    batch_gradient = output_gradient.reshape(blocks, KEY_BLOCK, HEAD_DIM).astype(jnp.float32)
    sums_b = log_sum.reshape(blocks, KEY_BLOCK)
    usable = picked >= 0
    safe_ids = jnp.maximum(picked, 0).astype(jnp.int32)
    far_span = SEL * KEY_BLOCK
    gathered_keys = jnp.concatenate([key_b[safe_ids].reshape(blocks, far_span, HEAD_DIM), key_b], axis=1)
    gathered_values = jnp.concatenate([value_b[safe_ids].reshape(blocks, far_span, HEAD_DIM), value_b], axis=1)
    far_mask = jnp.broadcast_to(jnp.repeat(usable, KEY_BLOCK, axis=1)[:, None, :], (blocks, KEY_BLOCK, far_span))
    lower_triangular = jnp.broadcast_to(jnp.tril(jnp.ones((KEY_BLOCK, KEY_BLOCK), dtype=bool)), (blocks, KEY_BLOCK, KEY_BLOCK))
    attend_mask = jnp.concatenate([far_mask, lower_triangular], axis=2)
    attention_scores = jnp.einsum("cjw,ctw->cjt", batch_query, gathered_keys) * scale_factor
    probs = jnp.where(attend_mask, jnp.exp(attention_scores - sums_b[:, :, None]), 0.0)
    probability_gradient = jnp.einsum("cjw,ctw->cjt", batch_gradient, gathered_values)
    row_dots = jnp.sum(probs * probability_gradient, axis=2)
    score_gradient = lax.optimization_barrier((probs * (probability_gradient - row_dots[:, :, None])).astype(jnp.bfloat16))
    reduced_probabilities = lax.optimization_barrier(probs.astype(jnp.bfloat16))
    query_gradient = (scale_factor * jnp.einsum("lzs,lsa->lza", score_gradient.astype(jnp.float32), gathered_keys)).astype(jnp.bfloat16)
    full_key_gradient = scale_factor * jnp.einsum("slm,slc->smc", score_gradient.astype(jnp.float32), batch_query)
    full_value_gradient = jnp.einsum("slm,slc->smc", reduced_probabilities.astype(jnp.float32), batch_gradient)
    flat_ids = safe_ids.reshape(-1)
    empty = jnp.zeros((blocks, KEY_BLOCK, HEAD_DIM), jnp.float32)
    grad_key = full_key_gradient[:, far_span:] + empty.at[flat_ids].add(full_key_gradient[:, :far_span].reshape(blocks * SEL, KEY_BLOCK, HEAD_DIM))
    grad_value = full_value_gradient[:, far_span:] + empty.at[flat_ids].add(full_value_gradient[:, :far_span].reshape(blocks * SEL, KEY_BLOCK, HEAD_DIM))
    return query_gradient.reshape(-1, HEAD_DIM), grad_key.reshape(-1, HEAD_DIM), grad_value.reshape(-1, HEAD_DIM)


def heads_first(array):
    return array.reshape(TOKENS, HEADS, HEAD_DIM).transpose(1, 0, 2)


def heads_back(array):
    return array.transpose(1, 0, 2).reshape(TOKENS, HEADS * HEAD_DIM)


def reference(query_rows, key_rows, value_rows, log_sums, cotangent, layer_input, chosen):
    query_gradient, grad_key, grad_value = lax.map(head_grads, (heads_first(query_rows), heads_first(key_rows), heads_first(value_rows), heads_first(cotangent), log_sums, chosen))
    grad_queries = heads_back(query_gradient)
    grad_weight = jnp.dot(layer_input.T, grad_queries, preferred_element_type=jnp.float32)
    return grad_queries, heads_back(grad_key), heads_back(grad_value), grad_weight
```

```python
import functools

import jax
import jax.numpy as jnp
from jax import lax
from jax.experimental import pallas as pl
from jax.experimental.pallas import tpu as pltpu
from jax.sharding import PartitionSpec as P

HEAD_DIM = 128
KEY_BLOCK = 32
CAP = 2
TILE = 256
SUB = 128
NEVER = -1e30


NT = (((1,), (1,)), ((), ()))
NN = (((1,), (0,)), ((), ()))
TN = (((0,), (0,)), ((), ()))


def dot(a, b, dims):
    return lax.dot_general(a, b, dims, preferred_element_type=jnp.float32)


def pick_body(ids_ref, key_ref, value_ref, out_ref):
    spans, heads = out_ref.shape[0], out_ref.shape[1]
    for head in range(heads):
        columns = slice(head * HEAD_DIM, (head + 1) * HEAD_DIM)

        def one(span, carry):
            for slot in range(CAP):
                start = pl.multiple_of(
                    ids_ref[slot, head * spans + span] * KEY_BLOCK, KEY_BLOCK
                )
                rows = pl.ds(start, KEY_BLOCK)
                to = slice(slot * KEY_BLOCK, (slot + 1) * KEY_BLOCK)
                out_ref[span, head, 0, to, :] = key_ref[rows, columns]
                out_ref[span, head, 1, to, :] = value_ref[rows, columns]
            return carry

        lax.fori_loop(0, spans, one, 0)


def pick(ids, key_rows, value_rows, spans, heads):
    return pl.pallas_call(
        pick_body,
        out_shape=jax.ShapeDtypeStruct(
            (spans, heads, 2, CAP * KEY_BLOCK, HEAD_DIM), jnp.bfloat16
        ),
        in_specs=[
            pl.BlockSpec(memory_space=pltpu.SMEM),
            pl.BlockSpec(memory_space=pltpu.VMEM),
            pl.BlockSpec(memory_space=pltpu.VMEM),
        ],
        out_specs=pl.BlockSpec(memory_space=pltpu.VMEM),
        name="pick_blocks",
    )(ids, key_rows, value_rows)


def attend_body(
    head,
    query_ref,
    key_ref,
    value_ref,
    cot_ref,
    sums_ref,
    far_ref,
    lists_ref,
    slots_ref,
    dq_ref,
    dk_ref,
    dv_ref,
    back_ref,
    acc_k,
    acc_v,
):
    step = pl.program_id(0)
    tile = query_ref.shape[0]
    spans = far_ref.shape[0]
    span_rows = CAP * KEY_BLOCK
    far_rows = (spans - 1) * span_rows
    scale = HEAD_DIM ** (-0.5)
    query = query_ref[...]
    cot = cot_ref[...]
    far_k = far_ref[: spans - 1, 0, 0].reshape(far_rows, HEAD_DIM)
    far_v = far_ref[: spans - 1, 0, 1].reshape(far_rows, HEAD_DIM)

    ids = slots_ref[0, : (spans - 1) * CAP, :]
    hit = lists_ref[0, 0:1, :] == ids
    for entry in range(1, lists_ref.shape[1]):
        hit = hit | (lists_ref[0, entry : entry + 1, :] == ids)
    far_bias = jnp.where(hit, 0.0, NEVER)
    far_bias = jnp.broadcast_to(
        far_bias[:, None, :], ((spans - 1) * CAP, KEY_BLOCK, tile)
    ).reshape(far_rows, tile)
    j = lax.broadcasted_iota(jnp.int32, (SUB, tile), 0)
    t = lax.broadcasted_iota(jnp.int32, (SUB, tile), 1) % SUB
    own_ok = (j // KEY_BLOCK == t // KEY_BLOCK) & (j <= t)
    own_bias = jnp.where(own_ok, 0.0, NEVER)

    parts = [slice(at, at + SUB) for at in range(0, tile, SUB)]
    own_s = jnp.concatenate([dot(key_ref[r, :], query[r, :], NT) for r in parts], axis=1)
    own_g = jnp.concatenate([dot(value_ref[r, :], cot[r, :], NT) for r in parts], axis=1)
    far_s = dot(far_k, query, NT)
    far_g = dot(far_v, cot, NT)
    sums = sums_ref[head : head + 1, :]
    far_p = jnp.exp(far_s * scale - sums + far_bias)
    own_p = jnp.exp(own_s * scale - sums + own_bias)
    row_dots = jnp.sum(far_p * far_g, axis=0, keepdims=True) + jnp.sum(
        own_p * own_g, axis=0, keepdims=True
    )
    far_d = (far_p * (far_g - row_dots)).astype(jnp.bfloat16)
    own_d = (own_p * (own_g - row_dots)).astype(jnp.bfloat16)
    far_low = far_p.astype(jnp.bfloat16)
    own_low = own_p.astype(jnp.bfloat16)

    far_q = dot(far_d, far_k, TN)
    for r in parts:
        dq = far_q[r, :] + dot(own_d[:, r], key_ref[r, :], TN)
        dq_ref[r, :] = (scale * dq).astype(jnp.bfloat16)
        dk_ref[r, :] = scale * dot(own_d[:, r], query[r, :], NN)
        dv_ref[r, :] = dot(own_low[:, r], cot[r, :], NN)
    step_k = dot(far_d, query, NN)
    step_v = dot(far_low, cot, NN)

    @pl.when(step == 0)
    def _():
        acc_k[...] = step_k
        acc_v[...] = step_v

    @pl.when(step > 0)
    def _():
        acc_k[...] += step_k
        acc_v[...] += step_v

    @pl.when(step == pl.num_programs(0) - 1)
    def _():
        shape = (spans - 1, span_rows, HEAD_DIM)
        back_ref[: spans - 1, 0] = (scale * acc_k[...]).astype(jnp.bfloat16).reshape(shape)
        back_ref[: spans - 1, 1] = acc_v[...].astype(jnp.bfloat16).reshape(shape)
        back_ref[spans - 1] = jnp.zeros((2, span_rows, HEAD_DIM), jnp.bfloat16)


def attend(head, query_rows, key_rows, value_rows, cotangent, log_sums, far, lists, slots):
    rows = query_rows.shape[0]
    spans = far.shape[0]
    heads = log_sums.shape[0]
    span_rows = CAP * KEY_BLOCK
    far_rows = (spans - 1) * span_rows
    tile = TILE
    column = pl.BlockSpec((tile, HEAD_DIM), lambda i: (i, head))
    single = pl.BlockSpec((tile, HEAD_DIM), lambda i: (i, 0))
    work = rows * (far_rows + SUB)
    return pl.pallas_call(
        functools.partial(attend_body, head),
        grid=(rows // tile,),
        out_shape=(
            jax.ShapeDtypeStruct((rows, HEAD_DIM), jnp.bfloat16),
            jax.ShapeDtypeStruct((rows, HEAD_DIM), jnp.float32),
            jax.ShapeDtypeStruct((rows, HEAD_DIM), jnp.float32),
            jax.ShapeDtypeStruct((spans, 2, span_rows, HEAD_DIM), jnp.bfloat16),
        ),
        in_specs=[
            column,
            column,
            column,
            column,
            pl.BlockSpec((heads, tile), lambda i: (0, i)),
            pl.BlockSpec((spans, 1, 2, span_rows, HEAD_DIM), lambda i: (0, head, 0, 0, 0)),
            pl.BlockSpec((1, lists.shape[1], tile), lambda i: (head, 0, i)),
            pl.BlockSpec((1, slots.shape[1], 1), lambda i: (head, 0, 0)),
        ],
        out_specs=(
            single,
            single,
            single,
            pl.BlockSpec((spans, 2, span_rows, HEAD_DIM), lambda i: (0, 0, 0, 0)),
        ),
        scratch_shapes=[
            pltpu.VMEM((far_rows, HEAD_DIM), jnp.float32),
            pltpu.VMEM((far_rows, HEAD_DIM), jnp.float32),
        ],
        cost_estimate=pl.CostEstimate(
            flops=10 * work * HEAD_DIM, bytes_accessed=rows * 2400, transcendentals=work
        ),
        name="attend_head",
    )(query_rows, key_rows, value_rows, cotangent, log_sums, far, lists, slots)


def land_body(heads, ids_ref, *refs):
    own_k, own_v, home = refs[:heads], refs[heads : 2 * heads], refs[2 * heads : 3 * heads]
    out_k, out_v = refs[3 * heads :]
    spans = home[0].shape[0]
    for head in range(heads):
        columns = slice(head * HEAD_DIM, (head + 1) * HEAD_DIM)
        out_k[:, columns] = own_k[head][...]
        out_v[:, columns] = own_v[head][...]

        def one(span, carry, head=head, columns=columns):
            for slot in range(CAP):
                start = pl.multiple_of(
                    ids_ref[slot, head * spans + span] * KEY_BLOCK, KEY_BLOCK
                )
                rows = pl.ds(start, KEY_BLOCK)
                at = slice(slot * KEY_BLOCK, (slot + 1) * KEY_BLOCK)
                out_k[rows, columns] += home[head][span, 0, at, :].astype(jnp.float32)
                out_v[rows, columns] += home[head][span, 1, at, :].astype(jnp.float32)
            return carry

        lax.fori_loop(1, spans, one, 0)


def land(ids, own_k, own_v, home):
    heads = len(own_k)
    rows = own_k[0].shape[0]
    whole = jax.ShapeDtypeStruct((rows, heads * HEAD_DIM), jnp.float32)
    return pl.pallas_call(
        functools.partial(land_body, heads),
        out_shape=(whole, whole),
        in_specs=[pl.BlockSpec(memory_space=pltpu.SMEM)]
        + [pl.BlockSpec(memory_space=pltpu.VMEM)] * (3 * heads),
        out_specs=(pl.BlockSpec(memory_space=pltpu.VMEM),) * 2,
        cost_estimate=pl.CostEstimate(
            flops=rows * heads, bytes_accessed=rows * heads * HEAD_DIM * 16, transcendentals=0
        ),
        name="land_blocks",
    )(ids, *own_k, *own_v, *home)


def hop(block, axis, bit, count):
    return lax.ppermute(block, axis, [(d, d ^ bit) for d in range(count)])


def spread(held, tp_count):
    bit = tp_count // 2
    order = [0, bit]
    bit //= 2
    while bit:
        held = held + [hop(piece, "tp", bit, tp_count) for piece in held]
        order = order + [m ^ bit for m in order]
        bit //= 2
    return [held[order.index(m)] for m in range(tp_count)]


def halves(rest, bit, kv_place):
    split = rest.reshape((-1, 2) + rest.shape[1:])
    mine = (kv_place & bit) != 0
    keep = jnp.where(mine, split[:, 1], split[:, 0])
    give = jnp.where(mine, split[:, 0], split[:, 1])
    return keep, give


def sum_scatter(pair, kv_count, kv_place):
    bit = 1
    while True:
        keep, give = pair
        came = hop(give, "kv", bit, kv_count)
        total = keep.astype(jnp.float32) + came.astype(jnp.float32)
        bit *= 2
        if bit == kv_count:
            return total.reshape(total.shape[1:])
        pair = halves(total.astype(jnp.bfloat16), bit, kv_place)


def local(query_rows, key_rows, value_rows, log_sums, cotangent, layer_input, chosen):
    kv_count = lax.axis_size("kv")
    tp_count = lax.axis_size("tp")
    kv_place = lax.axis_index("kv")
    tp_place = lax.axis_index("tp")
    heads = log_sums.shape[0]
    rows_here = query_rows.shape[0]
    blocks = rows_here // KEY_BLOCK
    chosen_count = chosen.shape[2]

    first = kv_place * blocks
    mine = (chosen >= first) & (chosen < first + blocks)
    asked = (heads, kv_count, blocks * chosen_count)
    low = jnp.min(jnp.where(mine, chosen - first, blocks).reshape(asked), axis=2)
    high = jnp.max(jnp.where(mine, chosen - first, -1).reshape(asked), axis=2)
    ids = jnp.stack([jnp.where(low == blocks, 0, low), jnp.maximum(high, 0)])
    ids = ids.reshape(CAP, heads * kv_count)
    sent = pick(ids, key_rows, value_rows, kv_count, heads)
    far = lax.all_to_all(sent, "kv", split_axis=0, concat_axis=0, tiled=True)

    own_lists = lax.dynamic_slice_in_dim(chosen, first, blocks, 1)
    flat_lists = own_lists.reshape(heads, 1, blocks * chosen_count)
    span_start = (jnp.arange(kv_count, dtype=jnp.int32) * blocks)[None, :, None]
    inside = (flat_lists >= span_start) & (flat_lists < span_start + blocks)
    want_low = jnp.min(jnp.where(inside, flat_lists, kv_count * blocks), axis=2)
    want_high = jnp.max(jnp.where(inside, flat_lists, -2), axis=2)
    want_high = jnp.where(want_high == want_low, -2, want_high)
    slots = jnp.stack([want_low, want_high], axis=2).reshape(heads, kv_count * CAP, 1)
    lists = jnp.repeat(jnp.swapaxes(own_lists, 1, 2), KEY_BLOCK, axis=2)

    own_k, own_v, queries, home = [], [], [], []
    for head in range(heads):
        dq, dk, dv, back = attend(
            head, query_rows, key_rows, value_rows, cotangent, log_sums, far, lists, slots
        )
        queries.append(dq)
        own_k.append(dk)
        own_v.append(dv)
        home.append(back)
    first_hop = tp_count // 2
    came = [hop(dq, "tp", first_hop, tp_count) for dq in queries]
    partial = []
    ready = queries[-1]
    for head in range(heads):
        came[head], ready = lax.optimization_barrier((came[head], ready))
        if head == 0:
            queries[-1] = ready
        else:
            partial[-1] = (partial[-1][0], ready)
        pieces = jnp.concatenate(spread([queries[head], came[head]], tp_count), axis=1)
        product = dot(layer_input, pieces, TN).astype(jnp.bfloat16)
        partial.append(halves(product.reshape(kv_count, -1, product.shape[1]), 1, kv_place))
        ready = partial[-1][1]
    partial = [sum_scatter(pair, kv_count, kv_place) for pair in partial]
    home = lax.all_to_all(
        jnp.stack(home, axis=1), "kv", split_axis=0, concat_axis=0, tiled=True
    )
    home = [home[:, head] for head in range(heads)]
    grad_keys, grad_values = land(ids, own_k, own_v, home)
    grad_queries = jnp.concatenate(queries, axis=1)

    weight = jnp.stack(
        [p.reshape(-1, tp_count, HEAD_DIM) for p in partial], axis=2
    )
    columns = [weight[:, m] for m in range(tp_count)]
    bit = 1
    while bit < tp_count:
        flip = (tp_place & bit) != 0
        columns = [
            jnp.where(flip, columns[m ^ bit], columns[m]) for m in range(tp_count)
        ]
        bit *= 2
    grad_weight = jnp.concatenate(
        [c.reshape(-1, heads * HEAD_DIM) for c in columns], axis=1
    )
    return (grad_queries, grad_keys, grad_values, grad_weight)


def solution(mesh):
    placed = (
        P("kv", "tp"),
        P("kv", "tp"),
        P("kv", "tp"),
        P("tp", "kv"),
        P("kv", "tp"),
        P("kv", "tp"),
        P("tp", None, None),
    )
    return jax.shard_map(
        local,
        mesh=mesh,
        in_specs=placed,
        out_specs=(P("kv", "tp"), P("kv", "tp"), P("kv", "tp"), P(("tp", "kv"), None)),
        check_vma=False,
    )
```
